32 devices in a mesh: sp: 16 (over z, y, x), tp: 2 (over core).
Axes of the slice: x: 2, y: 2, z: 4, core: 2. Of those that a mesh axis runs over, the one named last changes fastest.
Arguments:
- tokens: bfloat16 [4096, 2048], P('sp'), as said below
- in_gain: float32 [2048], replicated, may hold values from 0.1 to 1.9
- w_query: bfloat16 [2048, 1024], P(None, 'tp'), as said below
- w_key: bfloat16 [2048, 1024], P(None, 'tp'), may hold values from -0.125 to 0.125
- w_value: bfloat16 [2048, 1024], P(None, 'tp'), may hold values from -0.125 to 0.125
- lam: float32 [8], P('tp'), may hold values from 0.3 to 0.8
- sub_gain: float32 [128], replicated, may hold values from 0.1 to 1.9
- w_out: bfloat16 [1024, 2048], P('tp'), may hold values from -0.1875 to 0.1875
Outputs:
- mixed: bfloat16 [4096, 2048], P('sp')
The draws below stay inside these ranges and needn't reach their ends.
Inputs may be any that keep to these rules, and one draw needn't show every extreme that they name: tokens: normal entries plus, for each block of 64 tokens, a factor times one direction common to all tokens. w_query: independent normal entries.
All inputs are finite; a program needn't handle non-finite values.
Results may differ from the reference program's by a relative error of at most 0.025.
The reference program's roundings to bfloat16 on the way (of `normed`, `values`, `weights` and `attended`) count: a program that leaves them out, or rounds other values in their place, can miss the bound.
Values may be sent and summed in bfloat16 or wider, within the bound.
No kernel may reach another device: no remote copies, remote signals or barrier semaphores. Data moves between devices by JAX's collectives and lax.ppermute only.
A program may use at most 64 MiB of HBM per device.

```python
import jax
import jax.numpy as jnp
from jax import lax

D = 2048
HEADS = 8
KD = 64
VD = 128
TOKENS = 4096


def draw_tokens(key, part):
    first, second, third = jax.random.split(jax.random.fold_in(key, 11), 3)
    base = jax.random.normal(first, (TOKENS, D), jnp.float32)
    direction = jax.random.normal(second, (D,), jnp.float32)
    factor = jax.random.uniform(third, (TOKENS // 64,), jnp.float32, -1.5, 1.5)
    whole = base + jnp.repeat(factor, 64)[:, None] * direction[None, :]
    return jnp.clip(whole, -12.0, 12.0).astype(jnp.bfloat16)


def draw_w_query(key, part):
    base = jnp.clip(jax.random.normal(jax.random.fold_in(key, 23), (D, HEADS * 2 * KD), jnp.float32), -6.0, 6.0)
    scaled = base * (1.7 / jnp.sqrt(jnp.float32(D)))
    return scaled.astype(jnp.bfloat16)


def shard_levels(own_key, shape, shards, smallest, largest):
    gain = 1.0
    for axis_at, shards_of in shards:
        draws = jax.random.uniform(jax.random.fold_in(jax.random.fold_in(own_key, 6), axis_at), (shards_of,), jnp.float32, smallest / len(shards), largest / len(shards))
        gain = gain * jnp.repeat(jnp.exp(draws), shape[axis_at] // shards_of).reshape((-1,) + (1,) * (len(shape) - 1 - axis_at))
    return gain


def noise(key, shape, deviation, limit, cuts=(), held_as=jnp.bfloat16):
    drawn = deviation * jax.random.normal(key, shape, jnp.float32)
    if cuts:
        drawn = drawn * shard_levels(key, shape, cuts, -0.22, 0.18)
    return jnp.clip(drawn, -limit, limit).astype(held_as)


def setup_inputs(seed: int = 0) -> dict:
    streams_of = jax.random.split(jax.random.key(seed), 9)
    return {
        "tokens": draw_tokens(jax.random.fold_in(streams_of[8], 71), 0),
        "in_gain": jnp.clip(1.0 + 0.18 * jax.random.normal(streams_of[1], (D,), jnp.float32), 0.1, 1.9),
        "w_query": draw_w_query(jax.random.fold_in(streams_of[8], 71), 0),
        "w_key": noise(streams_of[3], (D, HEADS * 2 * KD), D ** -0.5, 0.125, ((1, 2),)),
        "w_value": noise(streams_of[4], (D, HEADS * VD), D ** -0.5, 0.125, ((1, 2),)),
        "lam": jnp.clip(0.3 + 0.5 * jax.random.uniform(streams_of[5], (HEADS,), jnp.float32) ** shard_levels(streams_of[5], (HEADS,), ((0, 2),), -0.2, 0.2), 0.3, 0.8),
        "sub_gain": jnp.clip(1.0 + 0.18 * jax.random.normal(streams_of[6], (VD,), jnp.float32), 0.1, 1.9),
        "w_out": noise(streams_of[7], (HEADS * VD, D), (HEADS * VD) ** -0.5, 0.1875, ((0, 2),)),
    }


def rotate(vectors, position):
    half = vectors.shape[-1] // 2
    freq = 500000.0 ** (-jnp.arange(0, 2 * half, 2, dtype=jnp.float32) / (2 * half))
    angle = position.astype(jnp.float32)[:, None] * freq[None, :]
    cosine = jnp.cos(angle)[:, None, :]
    sine = jnp.sin(angle)[:, None, :]
    first = vectors[..., :half]
    second = vectors[..., half:]
    return jnp.concatenate([first * cosine - second * sine, second * cosine + first * sine], axis=-1)

def reference(tokens, in_gain, w_query, w_key, w_value, lam, sub_gain, w_out):
    total = tokens.shape[0]
    xfloat = tokens.astype(jnp.float32)
    normed = (xfloat * lax.rsqrt(lax.optimization_barrier(jnp.mean(xfloat * xfloat, axis=-1, keepdims=True)) + 1e-06) * in_gain).astype(jnp.bfloat16)
    position = jnp.arange(total, dtype=jnp.int32)
    queries = rotate(jnp.dot(normed, w_query, preferred_element_type=jnp.float32).reshape(total, 2 * HEADS, KD), position).astype(jnp.bfloat16)
    keys = rotate(jnp.dot(normed, w_key, preferred_element_type=jnp.float32).reshape(total, 2 * HEADS, KD), position).astype(jnp.bfloat16)
    values = jnp.dot(normed, w_value, preferred_element_type=jnp.float32).astype(jnp.bfloat16).reshape(total, HEADS, VD)
    queries = jnp.transpose(queries.reshape(total, HEADS, 2, KD), (1, 0, 2, 3))
    keys = jnp.transpose(keys.reshape(total, HEADS, 2, KD), (1, 0, 2, 3))
    values = jnp.transpose(values, (1, 0, 2))
    block = min(512, total)
    scale = KD ** (-0.5)

    def one_head(items):
        query_h, key_h, value_h, lam_h = items
        keyf = key_h.astype(jnp.float32)
        valuef = value_h.astype(jnp.float32)

        def one_block(query_b):
            scores = jnp.einsum('qcd,kcd->cqk', query_b.astype(jnp.float32), keyf) * scale
            top = lax.optimization_barrier(jnp.max(scores, axis=-1, keepdims=True))
            expo = jnp.exp(scores - top)
            mass = lax.optimization_barrier(jnp.sum(expo, axis=-1))
            weights = expo.astype(jnp.bfloat16).astype(jnp.float32)
            read = jnp.einsum('cqk,ke->cqe', weights, valuef) / mass[..., None]
            diff = read[0] - lam_h * read[1]
            normal = diff * lax.rsqrt(lax.optimization_barrier(jnp.mean(diff * diff, axis=-1, keepdims=True)) + 1e-05) * sub_gain
            return normal.astype(jnp.bfloat16)
        blocks = query_h.reshape(total // block, block, 2, KD)
        return lax.map(one_block, blocks).reshape(total, VD)
    heads = lax.map(one_head, (queries, keys, values, lam))
    attended = jnp.transpose(heads, (1, 0, 2)).reshape(total, HEADS * VD)
    return jnp.dot(attended, w_out, preferred_element_type=jnp.float32).astype(jnp.bfloat16)
```

```python
import functools

import jax
import jax.numpy as jnp
from jax import lax
from jax.experimental import pallas as pl
from jax.experimental.pallas import tpu as pltpu
from jax.sharding import PartitionSpec as P

KD = 64
VD = 128
LOG2E = 1.4426950408889634
F32 = jnp.float32
BF16 = jnp.bfloat16
VMEM_LIMIT = 58 * 1024 * 1024


def whole_spec():
    return pl.BlockSpec(memory_space=pltpu.VMEM)


def smem_spec():
    return pl.BlockSpec(memory_space=pltpu.SMEM)


def halves(block):
    return jnp.concatenate(
        [block[:, at : at + 128] for at in range(0, block.shape[1], 128)], axis=0
    )


def unhalve(block):
    return jnp.concatenate(
        [block[at : at + 128, :] for at in range(0, block.shape[0], 128)], axis=1
    )


def project_body(zi, x, gain, cosine, sine, wq, wk, wv, *rest):
    outs, normed = rest[:-1], rest[-1]
    at = pl.program_id(0)
    span = x.shape[0]

    @pl.when(at == 0)
    def _():
        xf = x[...].astype(F32)
        inv = lax.rsqrt(jnp.mean(xf * xf, axis=-1, keepdims=True) + 1e-06)
        normed[...] = (xf * inv * gain[...]).astype(BF16)

    n = normed[...]
    qk = jnp.dot(n, jnp.concatenate([wq[...], wk[...]], axis=1), preferred_element_type=F32)
    v = jnp.dot(n, wv[...], preferred_element_type=F32)
    low = lax.broadcasted_iota(jnp.int32, (span, 2 * KD), 1) % KD < KD // 2

    def rotate(a):
        other = jnp.where(low, pltpu.roll(a, 2 * KD - KD // 2, 1), pltpu.roll(a, KD // 2, 1))
        return a * cosine[...] + other * sine[...]

    k = rotate(qk[:, 2 * KD :]).astype(BF16)
    vt = halves(v.T.astype(BF16))
    qt = halves(rotate(qk[:, : 2 * KD]).T.astype(BF16))
    for index, out in enumerate(outs):

        @pl.when(at == index)
        def _():
            out[0:span] = k
            out[span : 2 * span] = vt
            out[2 * span : 3 * span] = qt


def project(zi, tokens, in_gain, cosine, sine, w_query, w_key, w_value, heads):
    span, width = tokens.shape
    fixed = lambda i, z: (0, 0)
    weight = pl.BlockSpec((width, VD), lambda i, z: (0, jnp.bitwise_xor(z[0], i)))
    return pl.pallas_call(
        project_body,
        grid_spec=pltpu.PrefetchScalarGridSpec(
            num_scalar_prefetch=1,
            grid=(heads,),
            in_specs=[
                pl.BlockSpec((span, width), fixed),
                pl.BlockSpec((1, width), fixed),
                pl.BlockSpec((span, 2 * KD), fixed),
                pl.BlockSpec((span, 2 * KD), fixed),
                weight,
                weight,
                weight,
            ],
            out_specs=[pl.BlockSpec((3 * span, VD), fixed)] * heads,
            scratch_shapes=[pltpu.VMEM((span, width), BF16)],
        ),
        out_shape=[jax.ShapeDtypeStruct((3 * span, VD), BF16)] * heads,
        compiler_params=pltpu.CompilerParams(
            dimension_semantics=("arbitrary",), vmem_limit_bytes=VMEM_LIMIT
        ),
        name="project",
    )(zi, tokens, in_gain[None, :], cosine, sine, w_query, w_key, w_value)


def attend_body(*refs, nq, span, counts, first, last):
    refs = list(refs)
    take = lambda n: [refs.pop(0) for _ in range(n)]
    qs = take(nq)
    kvs = take(len(counts))
    carry_in = [] if first else take(3)
    extra = take(2) if last else []
    outs = take(nq) if last else take(3)
    kscr, vscr, qscr, sscr = take(4)
    blocks = 2 * nq
    total = sum(counts)
    pair = vscr.shape[2] // span
    step = pair * span
    steps = total // pair

    at = 0
    for kv, count in zip(kvs, counts):
        for j in range(count):
            kscr[at * span : (at + 1) * span] = kv[j, 0:span]
            vscr[at // pair, :, (at % pair) * span : (at % pair + 1) * span] = unhalve(
                kv[j, span : 2 * span]
            )
            at += 1
    row = lax.broadcasted_iota(jnp.int32, (2 * KD, span), 0) < KD
    for d in range(nq):
        q = unhalve(qs[d][2 * span : 3 * span]).astype(F32) * (KD**-0.5 * LOG2E)
        high = q.astype(BF16)
        rest = (q - high.astype(F32)).astype(BF16)
        zero = jnp.zeros_like(high)
        for c in range(2):
            mask = row if c == 0 else jnp.logical_not(row)
            qscr[2 * d + c, 0 : 2 * KD] = jnp.where(mask, high, zero)
            qscr[2 * d + c, 2 * KD : 4 * KD] = jnp.where(mask, rest, zero)

    def groups(a):
        return a.reshape(a.shape[0] // 8, 8, a.shape[1])

    def score(b, slot, i, m8):
        k = kscr[pl.ds(pl.multiple_of(i * step, step), step), :]
        s = jnp.dot(jnp.concatenate([k, k], axis=1), qscr[b], preferred_element_type=F32)
        sscr[slot, pl.ds(pl.multiple_of(i * step, step), step), :] = s
        return jnp.maximum(m8, jnp.max(groups(s), axis=0))

    def spread(m8):
        return jnp.broadcast_to(jnp.max(m8, axis=0, keepdims=True), m8.shape)

    low = jnp.full((8, span), -1e30, F32)
    zero8 = jnp.zeros((8, span), F32)
    state = []
    m8 = lax.fori_loop(0, steps, lambda i, m: score(0, 0, i, m), low if first else carry_in[0][0])
    for b in range(blocks):
        m = spread(m8)
        if first:
            mass0 = zero8
            acc0 = jnp.zeros((VD, span), F32)
        else:
            fix = jnp.exp2(carry_in[0][b] - m)
            mass0 = carry_in[1][b] * fix
            acc0 = (groups(carry_in[2][b]) * fix[None]).reshape(VD, span)

        def body(i, carry, b=b, m=m):
            next8, mass, acc = carry
            s = sscr[b % 2, pl.ds(pl.multiple_of(i * step, step), step), :]
            p = jnp.exp2(groups(s) - m[None])
            mass = mass + jnp.sum(p, axis=0)
            acc = acc + jnp.dot(
                vscr[i], p.reshape(step, span).astype(BF16), preferred_element_type=F32
            )
            if b + 1 < blocks:
                next8 = score(b + 1, (b + 1) % 2, i, next8)
            return next8, mass, acc

        next0 = low if first or b + 1 == blocks else carry_in[0][b + 1]
        m8, mass, acc = lax.fori_loop(0, steps, body, (next0, mass0, acc0))
        if not last:
            outs[0][b] = m
            outs[1][b] = mass
            outs[2][b] = acc
            continue
        read = acc / jnp.sum(mass, axis=0, keepdims=True)
        if b % 2 == 0:
            state = read
        else:
            lam, gain = extra
            diff = state - lam[0] * read
            inv = lax.rsqrt(jnp.mean(diff * diff, axis=0, keepdims=True) + 1e-05)
            outs[b // 2][...] = (diff * inv * gain[...]).T.astype(BF16)


def attend(qs, kvs, carry, finish, span):
    nq = len(qs)
    counts = tuple(kv.shape[0] for kv in kvs)
    total = sum(counts)
    pair = next(n for n in (4, 2, 1) if total % n == 0)
    blocks = 2 * nq
    first, last = carry is None, finish is not None
    args = [*qs, *kvs, *(carry or ()), *(finish or ())]
    specs = [whole_spec() for _ in args]
    if last:
        specs[-2] = smem_spec()
        out_shape = [jax.ShapeDtypeStruct((span, VD), BF16)] * nq
    else:
        out_shape = [
            jax.ShapeDtypeStruct((blocks, 8, span), F32),
            jax.ShapeDtypeStruct((blocks, 8, span), F32),
            jax.ShapeDtypeStruct((blocks, VD, span), F32),
        ]
    return pl.pallas_call(
        functools.partial(
            attend_body, nq=nq, span=span, counts=counts, first=first, last=last
        ),
        in_specs=specs,
        out_specs=[whole_spec() for _ in out_shape],
        out_shape=out_shape,
        scratch_shapes=[
            pltpu.VMEM((total * span, VD), BF16),
            pltpu.VMEM((total // pair, VD, pair * span), BF16),
            pltpu.VMEM((blocks, 4 * KD, span), BF16),
            pltpu.VMEM((2, total * span, span), F32),
        ],
        compiler_params=pltpu.CompilerParams(vmem_limit_bytes=VMEM_LIMIT),
        name="attend",
    )(*args)


def output_body(zi, *refs):
    out, scr = refs[-2:]
    weights = refs[-4:-2]
    pieces = refs[:-4]
    heads = len(pieces) // 2

    @pl.when(pl.program_id(0) == 0)
    def _():
        for index, piece in enumerate(pieces):
            side, d = divmod(index, heads)
            head = jnp.bitwise_xor(zi[0], d)
            scr[side, :, pl.ds(pl.multiple_of(head * VD, VD), VD)] = piece[...]

    total = jnp.dot(scr[0], weights[0][...], preferred_element_type=F32)
    total = total + jnp.dot(scr[1], weights[1][...], preferred_element_type=F32)
    out[...] = total.astype(BF16)


def output(zi, own, other, w_own, w_other):
    span = own[0].shape[0]
    rows, width = w_own.shape
    tile = 512
    fixed = lambda i, z: (0, 0)
    piece = pl.BlockSpec((span, VD), fixed)
    weight = pl.BlockSpec((rows, tile), lambda i, z: (0, i))
    return pl.pallas_call(
        output_body,
        grid_spec=pltpu.PrefetchScalarGridSpec(
            num_scalar_prefetch=1,
            grid=(width // tile,),
            in_specs=[piece] * (2 * len(own)) + [weight, weight],
            out_specs=pl.BlockSpec((span, tile), lambda i, z: (0, i)),
            scratch_shapes=[pltpu.VMEM((2, span, rows), BF16)],
        ),
        out_shape=jax.ShapeDtypeStruct((span, width), BF16),
        compiler_params=pltpu.CompilerParams(
            dimension_semantics=("arbitrary",), vmem_limit_bytes=VMEM_LIMIT
        ),
        name="output",
    )(zi, *own, *other, w_own, w_other)


def shards(tokens, in_gain, w_query, w_key, w_value, lam, sub_gain, w_out, *, size, tp):
    span = tokens.shape[0]
    heads = lam.shape[0]
    split = heads if heads & (heads - 1) == 0 and size % heads == 0 else 1
    rest = size // split
    where = lax.axis_index("sp")
    zi = where // rest

    def swap_far(a, d):
        return lax.ppermute(
            a, "sp", [(i, ((i // rest) ^ d) * rest + i % rest) for i in range(size)]
        )

    def swap_near(a, d):
        return lax.ppermute(a, "sp", [(i, i ^ d) for i in range(size)])

    position = (where * span + jnp.arange(span, dtype=jnp.int32)).astype(F32)
    freq = 500000.0 ** (-jnp.arange(0, KD, 2, dtype=F32) / KD)
    angle = position[:, None] * freq[None, :]
    cosine, sine = jnp.cos(angle), jnp.sin(angle)
    cosine = jnp.concatenate([cosine] * 4, axis=1)
    sine = jnp.concatenate([-sine, sine, -sine, sine], axis=1)
    index = zi.astype(jnp.int32)[None] if split == heads else jnp.zeros((1,), jnp.int32)
    parts = project(index, tokens, in_gain, cosine, sine, w_query, w_key, w_value, heads)
    gain = sub_gain[:, None]

    if split == heads:
        mine = [parts[0]] + [None] * (heads - 1)
        for d in sorted(range(1, heads), key=lambda n: -(n ^ 1)):
            mine[d] = swap_far(parts[d], d)
        kv = jnp.stack([a[: 2 * span] for a in mine])
        if rest == 4:
            half = heads // 2 if heads > 1 else 1
            left, right = swap_near(kv, 1), swap_near(kv, 2)
            cross = [swap_near(left[:half], 2)]
            if heads > 1:
                cross.append(swap_near(right[half:], 1))
            pieces = [[kv, left, right, *cross]]
        else:
            groups = [[g * rest + r for r in range(rest)] for g in range(split)]
            kw = {} if split == 1 else {"axis_index_groups": groups}
            every = lax.all_gather(kv, "sp", axis=0, tiled=True, **kw)
            pieces = [[every[at : at + 16]] for at in range(0, every.shape[0], 16)]
        lam_mine = lax.dynamic_slice_in_dim(lam, index[0], 1)
        carry = None
        for at, piece in enumerate(pieces):
            finish = (lam_mine, gain) if at + 1 == len(pieces) else None
            carry = attend(mine, piece, carry, finish, span)
        own = [carry[0]] + [swap_far(carry[d], d) for d in range(1, heads)]
    else:
        own = []
        for h in range(heads):
            every = lax.all_gather(parts[h][None, : 2 * span], "sp", axis=0, tiled=True)
            carry = None
            for at in range(0, size, 16):
                finish = (lam[h : h + 1], gain) if at + 16 >= size else None
                carry = attend([parts[h]], [every[at : at + 16]], carry, finish, span)
            own.append(carry[0])

    if tp == 2:
        flip = [(0, 1), (1, 0)]
        w_other = lax.ppermute(w_out, "tp", flip)
        other = [lax.ppermute(a, "tp", flip) for a in own]
        return output(index, own, other, w_out, w_other)
    attended = jnp.concatenate(own, axis=1)
    if tp > 1:
        attended = lax.all_gather(attended, "tp", axis=1, tiled=True)
        w_out = lax.all_gather(w_out, "tp", axis=0, tiled=True)
    return jnp.dot(attended, w_out, preferred_element_type=F32).astype(BF16)


def solution(mesh):
    in_specs = (
        P("sp", None),
        P(),
        P(None, "tp"),
        P(None, "tp"),
        P(None, "tp"),
        P("tp"),
        P(),
        P("tp", None),
    )
    body = functools.partial(shards, size=mesh.shape["sp"], tp=mesh.shape["tp"])
    return jax.shard_map(
        body, mesh=mesh, in_specs=in_specs, out_specs=P("sp", None), check_vma=False
    )
```

```python
import functools

import jax
import jax.numpy as jnp
from jax import lax
from jax.experimental import pallas as pl
from jax.experimental.pallas import tpu as pltpu
from jax.sharding import PartitionSpec as P

KD = 64
VD = 128
LOG2E = 1.4426950408889634
F32 = jnp.float32
BF16 = jnp.bfloat16
VMEM_LIMIT = 58 * 1024 * 1024


def whole_spec():
    return pl.BlockSpec(memory_space=pltpu.VMEM)


def smem_spec():
    return pl.BlockSpec(memory_space=pltpu.SMEM)


def halves(block):
    return jnp.concatenate(
        [block[:, at : at + 128] for at in range(0, block.shape[1], 128)], axis=0
    )


def unhalve(block):
    return jnp.concatenate(
        [block[at : at + 128, :] for at in range(0, block.shape[0], 128)], axis=1
    )


def project_body(zi, x, gain, cosine, sine, wq, wk, wv, *rest):
    outs, normed = rest[:-1], rest[-1]
    at = pl.program_id(0)
    span = x.shape[0]

    @pl.when(at == 0)
    def _():
        xf = x[...].astype(F32)
        inv = lax.rsqrt(jnp.mean(xf * xf, axis=-1, keepdims=True) + 1e-06)
        normed[...] = (xf * inv * gain[...]).astype(BF16)

    n = normed[...]
    qk = jnp.dot(n, jnp.concatenate([wq[...], wk[...]], axis=1), preferred_element_type=F32)
    v = jnp.dot(n, wv[...], preferred_element_type=F32)
    low = lax.broadcasted_iota(jnp.int32, (span, 2 * KD), 1) % KD < KD // 2

    def rotate(a):
        other = jnp.where(low, pltpu.roll(a, 2 * KD - KD // 2, 1), pltpu.roll(a, KD // 2, 1))
        return a * cosine[...] + other * sine[...]

    k = rotate(qk[:, 2 * KD :]).astype(BF16)
    vt = halves(v.T.astype(BF16))
    qt = halves(rotate(qk[:, : 2 * KD]).T.astype(BF16))
    for index, out in enumerate(outs):

        @pl.when(at == index)
        def _():
            out[0:span] = k
            out[span : 2 * span] = vt
            out[2 * span : 3 * span] = qt


def project(zi, tokens, in_gain, cosine, sine, w_query, w_key, w_value, heads):
    span, width = tokens.shape
    fixed = lambda i, z: (0, 0)
    weight = pl.BlockSpec((width, VD), lambda i, z: (0, jnp.bitwise_xor(z[0], i)))
    return pl.pallas_call(
        project_body,
        grid_spec=pltpu.PrefetchScalarGridSpec(
            num_scalar_prefetch=1,
            grid=(heads,),
            in_specs=[
                pl.BlockSpec((span, width), fixed),
                pl.BlockSpec((1, width), fixed),
                pl.BlockSpec((span, 2 * KD), fixed),
                pl.BlockSpec((span, 2 * KD), fixed),
                weight,
                weight,
                weight,
            ],
            out_specs=[pl.BlockSpec((3 * span, VD), fixed)] * heads,
            scratch_shapes=[pltpu.VMEM((span, width), BF16)],
        ),
        out_shape=[jax.ShapeDtypeStruct((3 * span, VD), BF16)] * heads,
        compiler_params=pltpu.CompilerParams(
            dimension_semantics=("arbitrary",), vmem_limit_bytes=VMEM_LIMIT
        ),
        name="project",
    )(zi, tokens, in_gain[None, :], cosine, sine, w_query, w_key, w_value)


def attend_body(*refs, nq, span, counts, first, last):
    refs = list(refs)
    take = lambda n: [refs.pop(0) for _ in range(n)]
    qs = take(nq)
    kvs = take(len(counts))
    carry_in = [] if first else take(3)
    extra = take(2) if last else []
    outs = take(nq) if last else take(3)
    kscr, vscr, qscr, sscr = take(4)
    total = sum(counts)
    pair = vscr.shape[2] // span
    step = pair * span
    steps = total // pair

    at = 0
    for kv, count in zip(kvs, counts):
        for j in range(count):
            kscr[at * span : (at + 1) * span] = kv[j, 0:span]
            vscr[at // pair, :, (at % pair) * span : (at % pair + 1) * span] = unhalve(
                kv[j, span : 2 * span]
            )
            at += 1
    row = lax.broadcasted_iota(jnp.int32, (2 * KD, span), 0) < KD
    for d in range(nq):
        q = unhalve(qs[d][2 * span : 3 * span]).astype(F32) * (KD**-0.5 * LOG2E)
        high = q.astype(BF16)
        rest = (q - high.astype(F32)).astype(BF16)
        zero = jnp.zeros_like(high)
        for c in range(2):
            mask = row if c == 0 else jnp.logical_not(row)
            cols = slice(c * span, (c + 1) * span)
            qscr[d, 0 : 2 * KD, cols] = jnp.where(mask, high, zero)
            qscr[d, 2 * KD : 4 * KD, cols] = jnp.where(mask, rest, zero)

    def groups(a):
        return a.reshape(a.shape[0] // 8, 8, a.shape[1])

    def score(d, i, m8):
        k = kscr[i * step : (i + 1) * step, :]
        s = jnp.dot(jnp.concatenate([k, k], axis=1), qscr[d], preferred_element_type=F32)
        sscr[d % 2, i * step : (i + 1) * step, :] = s
        return jnp.maximum(m8, jnp.max(groups(s), axis=0))

    low = jnp.full((8, 2 * span), -1e30, F32)
    m8 = low if first else carry_in[0][0]
    for i in range(steps):
        m8 = score(0, i, m8)
    for d in range(nq):
        m = jnp.broadcast_to(jnp.max(m8, axis=0, keepdims=True), m8.shape)
        if first:
            mass = jnp.zeros_like(m)
            acc = None
        else:
            fix = jnp.exp2(carry_in[0][d] - m)
            mass = carry_in[1][d] * fix
            acc = (groups(carry_in[2][d]) * fix[None]).reshape(VD, 2 * span)
        more = d + 1 < nq
        if more:
            m8 = low if first else carry_in[0][d + 1]
        for i in range(steps):
            p = jnp.exp2(groups(sscr[d % 2, i * step : (i + 1) * step, :]) - m[None])
            mass = mass + jnp.sum(p, axis=0)
            part = jnp.dot(
                vscr[i], p.reshape(step, 2 * span).astype(BF16), preferred_element_type=F32
            )
            acc = part if acc is None else acc + part
            if more:
                m8 = score(d + 1, i, m8)
        if not last:
            outs[0][d] = m
            outs[1][d] = mass
            outs[2][d] = acc
            continue
        lam, gain = extra
        read = acc / jnp.sum(mass, axis=0, keepdims=True)
        diff = read[:, :span] - lam[0] * read[:, span:]
        inv = lax.rsqrt(jnp.mean(diff * diff, axis=0, keepdims=True) + 1e-05)
        outs[d][...] = (diff * inv * gain[...]).T.astype(BF16)


def attend(qs, kvs, carry, finish, span):
    nq = len(qs)
    counts = tuple(kv.shape[0] for kv in kvs)
    total = sum(counts)
    pair = next(n for n in (4, 2, 1) if total % n == 0)
    first, last = carry is None, finish is not None
    args = [*qs, *kvs, *(carry or ()), *(finish or ())]
    specs = [whole_spec() for _ in args]
    if last:
        specs[-2] = smem_spec()
        out_shape = [jax.ShapeDtypeStruct((span, VD), BF16)] * nq
    else:
        out_shape = [
            jax.ShapeDtypeStruct((nq, 8, 2 * span), F32),
            jax.ShapeDtypeStruct((nq, 8, 2 * span), F32),
            jax.ShapeDtypeStruct((nq, VD, 2 * span), F32),
        ]
    return pl.pallas_call(
        functools.partial(
            attend_body, nq=nq, span=span, counts=counts, first=first, last=last
        ),
        in_specs=specs,
        out_specs=[whole_spec() for _ in out_shape],
        out_shape=out_shape,
        scratch_shapes=[
            pltpu.VMEM((total * span, VD), BF16),
            pltpu.VMEM((total // pair, VD, pair * span), BF16),
            pltpu.VMEM((nq, 4 * KD, 2 * span), BF16),
            pltpu.VMEM((2, total * span, 2 * span), F32),
        ],
        compiler_params=pltpu.CompilerParams(vmem_limit_bytes=VMEM_LIMIT),
        name="attend",
    )(*args)


def output_body(zi, *refs):
    out, scr = refs[-2:]
    weights = refs[-4:-2]
    pieces = refs[:-4]
    heads = len(pieces) // 2

    @pl.when(pl.program_id(0) == 0)
    def _():
        for index, piece in enumerate(pieces):
            side, d = divmod(index, heads)
            head = jnp.bitwise_xor(zi[0], d)
            scr[side, :, pl.ds(pl.multiple_of(head * VD, VD), VD)] = piece[...]

    total = jnp.dot(scr[0], weights[0][...], preferred_element_type=F32)
    total = total + jnp.dot(scr[1], weights[1][...], preferred_element_type=F32)
    out[...] = total.astype(BF16)


def output(zi, own, other, w_own, w_other):
    span = own[0].shape[0]
    rows, width = w_own.shape
    tile = 512
    fixed = lambda i, z: (0, 0)
    piece = pl.BlockSpec((span, VD), fixed)
    weight = pl.BlockSpec((rows, tile), lambda i, z: (0, i))
    return pl.pallas_call(
        output_body,
        grid_spec=pltpu.PrefetchScalarGridSpec(
            num_scalar_prefetch=1,
            grid=(width // tile,),
            in_specs=[piece] * (2 * len(own)) + [weight, weight],
            out_specs=pl.BlockSpec((span, tile), lambda i, z: (0, i)),
            scratch_shapes=[pltpu.VMEM((2, span, rows), BF16)],
        ),
        out_shape=jax.ShapeDtypeStruct((span, width), BF16),
        compiler_params=pltpu.CompilerParams(
            dimension_semantics=("arbitrary",), vmem_limit_bytes=VMEM_LIMIT
        ),
        name="output",
    )(zi, *own, *other, w_own, w_other)


def shards(tokens, in_gain, w_query, w_key, w_value, lam, sub_gain, w_out, *, size, tp):
    span = tokens.shape[0]
    heads = lam.shape[0]
    split = heads if heads & (heads - 1) == 0 and size % heads == 0 else 1
    rest = size // split
    where = lax.axis_index("sp")
    flip = [(0, 1), (1, 0)]
    zi = where // rest

    def swap_far(a, d):
        return lax.ppermute(
            a, "sp", [(i, ((i // rest) ^ d) * rest + i % rest) for i in range(size)]
        )

    def swap_near(a, d):
        return lax.ppermute(a, "sp", [(i, i ^ d) for i in range(size)])

    position = (where * span + jnp.arange(span, dtype=jnp.int32)).astype(F32)
    freq = 500000.0 ** (-jnp.arange(0, KD, 2, dtype=F32) / KD)
    angle = position[:, None] * freq[None, :]
    cosine, sine = jnp.cos(angle), jnp.sin(angle)
    cosine = jnp.concatenate([cosine] * 4, axis=1)
    sine = jnp.concatenate([-sine, sine, -sine, sine], axis=1)
    index = zi.astype(jnp.int32)[None] if split == heads else jnp.zeros((1,), jnp.int32)
    parts = project(index, tokens, in_gain, cosine, sine, w_query, w_key, w_value, heads)
    gain = sub_gain[:, None]

    if split == heads:
        swapped = tp == 2 and rest == 4
        lam_here = lam
        if swapped:
            lam_other = lax.ppermute(lam, "tp", flip)
            same = (where % 4) // 2 == lax.axis_index("tp")
            lam_here = jnp.where(same, lam, lam_other)

            def far(a, d):
                pairs = []
                for i in range(size):
                    z, y, x = i // 4, (i // 2) % 2, i % 2
                    for t in range(2):
                        pairs.append((2 * i + t, 2 * ((z ^ d) * 4 + t * 2 + x) + y))
                return lax.ppermute(a, ("sp", "tp"), pairs)

            mine = [None] * heads
            for d in [0] + sorted(range(1, heads), key=lambda n: -(n ^ 1)):
                mine[d] = far(parts[d], d)
        else:
            far = swap_far
            mine = [parts[0]] + [far(parts[d], d) for d in range(1, heads)]
        lam_mine = lax.dynamic_slice_in_dim(lam_here, index[0], 1)
        kv = [a[None, : 2 * span] for a in mine]
        finish = (lam_mine, gain)
        if swapped and heads == 4:
            cross_core = lambda a: lax.ppermute(a, "tp", flip)
            one = jnp.concatenate([kv[0], kv[2]], axis=0)
            two = jnp.concatenate([kv[3], kv[1]], axis=0)
            far_one = swap_near(one, 1)
            far_two = swap_near(two, 1)
            side_one, side_two = cross_core(one), cross_core(two)
            far_side_one = cross_core(far_one)
            far_side_two = cross_core(far_two)
            carry = attend(mine, [one, two], None, None, span)
            carry = attend(mine, [side_one, side_two], carry, None, span)
            carry = attend(mine, [far_one, far_side_one], carry, None, span)
            own = [None] * 4
            for picks in ([2, 3], [1, 0]):
                some = [
                    jnp.concatenate([c[n : n + 1] for n in picks], axis=0) for c in carry
                ]
                done = attend([mine[n] for n in picks], [far_two, far_side_two], some, finish, span)
                for n, a in zip(picks, done):
                    own[n] = far(a, n)
        else:
            kv = jnp.concatenate(kv, axis=0)
            groups = [[g * rest + r for r in range(rest)] for g in range(split)]
            kw = {} if split == 1 else {"axis_index_groups": groups}
            every = lax.all_gather(kv, "sp", axis=0, tiled=True, **kw)
            carry = None
            for at in range(0, every.shape[0], 8):
                end = finish if at + 8 >= every.shape[0] else None
                carry = attend(mine, [every[at : at + 8]], carry, end, span)
            own = [carry[0]] + [far(carry[d], d) for d in range(1, heads)]
    else:
        own = []
        for h in range(heads):
            every = lax.all_gather(parts[h][None, : 2 * span], "sp", axis=0, tiled=True)
            carry = None
            for at in range(0, size, 8):
                end = (lam[h : h + 1], gain) if at + 8 >= size else None
                carry = attend([parts[h]], [every[at : at + 8]], carry, end, span)
            own.append(carry[0])

    if tp == 2:
        w_other = lax.ppermute(w_out, "tp", flip)
        other = lax.ppermute(jnp.stack(own), "tp", flip)
        other = [other[d] for d in range(heads)]
        return output(index, own, other, w_out, w_other)
    attended = jnp.concatenate(own, axis=1)
    if tp > 1:
        attended = lax.all_gather(attended, "tp", axis=1, tiled=True)
        w_out = lax.all_gather(w_out, "tp", axis=0, tiled=True)
    return jnp.dot(attended, w_out, preferred_element_type=F32).astype(BF16)


def solution(mesh):
    in_specs = (
        P("sp", None),
        P(),
        P(None, "tp"),
        P(None, "tp"),
        P(None, "tp"),
        P("tp"),
        P(),
        P("tp", None),
    )
    body = functools.partial(shards, size=mesh.shape["sp"], tp=mesh.shape["tp"])
    return jax.shard_map(
        body, mesh=mesh, in_specs=in_specs, out_specs=P("sp", None), check_vma=False
    )
```

```python
import functools

import jax
import jax.numpy as jnp
from jax import lax
from jax.experimental import pallas as pl
from jax.experimental.pallas import tpu as pltpu
from jax.sharding import PartitionSpec as P


KD = 64
VD = 128
LOG2E = 1.4426950408889634
LOG2_BASE = 18.931568569324174
F32 = jnp.float32
BF16 = jnp.bfloat16
MIB = 1024 * 1024


def whole_spec():
    return pl.BlockSpec(memory_space=pltpu.VMEM)


def smem_spec():
    return pl.BlockSpec(memory_space=pltpu.SMEM)


def halves(block):
    return jnp.concatenate(
        [block[:, at : at + 128] for at in range(0, block.shape[1], 128)], axis=0
    )


def unhalve(block):
    return jnp.concatenate(
        [block[at : at + 128, :] for at in range(0, block.shape[0], 128)], axis=1
    )


def project_body(place, x_hbm, gain, *rest):
    weights = rest[:3]
    out, xv, wv, normed, sem_x, sem_w = rest[3:]
    span, width = xv.shape
    heads = out.shape[0]
    pieces = sem_w.shape[1]
    rows = width // pieces
    loads = []
    x_copy = pltpu.make_async_copy(x_hbm, xv, sem_x)
    x_copy.start()
    for w in range(3):
        loads.append([])
        for j in range(pieces):
            part = pl.ds(j * rows, rows)
            copy = pltpu.make_async_copy(
                weights[w].at[part, :], wv.at[w, part, :], sem_w.at[w, j]
            )
            copy.start()
            loads[w].append(copy)

    lane = lax.broadcasted_iota(jnp.int32, (1, 2 * KD), 1)
    low = lane % KD < KD // 2
    freq = jnp.exp2((lane % (KD // 2)).astype(F32) * (-2.0 * LOG2_BASE / KD))
    half = KD // 2
    many = 2 * KD // half
    deep = span // many
    position = (
        place[1]
        + lax.broadcasted_iota(jnp.int32, (deep, 2 * KD), 0)
        + lax.broadcasted_iota(jnp.int32, (deep, 2 * KD), 1) // half * deep
    )
    angle = position.astype(F32) * freq

    def spread(table):
        blocks = []
        for g in range(many):
            block = jnp.where(lane // half == g, table, 0.0)
            block = block + pltpu.roll(block, half, 1)
            blocks.append(block + pltpu.roll(block, 2 * half, 1))
        return jnp.concatenate(blocks, axis=0)

    cosine = spread(jnp.cos(angle))
    sine = spread(jnp.sin(angle))
    sine = jnp.where(low, -sine, sine)

    x_copy.wait()
    xf = xv[...].astype(F32)
    inv = lax.rsqrt(jnp.mean(xf * xf, axis=-1, keepdims=True) + 1e-06)
    normed[...] = (xf * inv * gain[...]).astype(BF16)

    def times(w):
        for copy in loads[w]:
            copy.wait()
        return jnp.dot(normed[...], wv[w], preferred_element_type=F32)

    def rotate(a):
        other = jnp.where(low, pltpu.roll(a, 2 * KD - KD // 2, 1), pltpu.roll(a, KD // 2, 1))
        return a * cosine + other * sine

    tile = lambda a, h: a[:, h * VD : (h + 1) * VD]
    slot = lambda h: jnp.bitwise_xor(place[0], h)
    k = times(0)
    for h in range(heads):
        out[slot(h), 0:span] = rotate(tile(k, h)).astype(BF16)
    v = times(1)
    for h in range(heads):
        out[slot(h), span : 2 * span] = halves(tile(v, h).T.astype(BF16))
    q = times(2)
    for h in range(heads):
        out[slot(h), 2 * span : 3 * span] = halves(rotate(tile(q, h)).T.astype(BF16))


def project(place, tokens, in_gain, w_query, w_key, w_value, heads):
    span, width = tokens.shape
    cols = w_query.shape[1]
    hbm = pl.BlockSpec(memory_space=pltpu.HBM)
    return pl.pallas_call(
        project_body,
        in_specs=[smem_spec(), hbm, whole_spec(), hbm, hbm, hbm],
        out_specs=whole_spec(),
        scratch_shapes=[
            pltpu.VMEM((span, width), BF16),
            pltpu.VMEM((3, width, cols), BF16),
            pltpu.VMEM((span, width), BF16),
            pltpu.SemaphoreType.DMA(()),
            pltpu.SemaphoreType.DMA((3, 4)),
        ],
        out_shape=jax.ShapeDtypeStruct((heads, 3 * span, VD), BF16),
        cost_estimate=pl.CostEstimate(
            flops=6 * span * width * cols, transcendentals=0, bytes_accessed=6 * width * cols
        ),
        compiler_params=pltpu.CompilerParams(vmem_limit_bytes=115 * MIB // 2),
        name="project",
    )(place, tokens, in_gain[None, :], w_key, w_value, w_query)


def attend_body(*refs, nq, span, counts, first, last):
    refs = list(refs)
    take = lambda n: [refs.pop(0) for _ in range(n)]
    qs = take(nq)
    kvs = take(len(counts))
    carry_in = [] if first else take(3)
    extra = take(2) if last else []
    outs = take(1) if last else take(3)
    kscr, vscr, qscr, sscr = take(4)
    total = sum(counts)
    keys = total * span
    wide = 2 * span

    at = 0
    for kv, count in zip(kvs, counts):

        def load(j, none, kv=kv, at=at):
            kscr[pl.ds(pl.multiple_of((at + j) * span, span), span), :] = kv[j, 0:span]
            cols = pl.ds(pl.multiple_of((at + j) * span, span), span)
            vscr[:, cols] = unhalve(kv[j, span : 2 * span])
            return none

        lax.fori_loop(0, count, load, 0)
        at += count
    row = lax.broadcasted_iota(jnp.int32, (2 * KD, span), 0) < KD
    for d in range(nq):
        q = unhalve(qs[d][2 * span : 3 * span])
        for c in range(2):
            mask = row if c == 0 else jnp.logical_not(row)
            qscr[d, :, c * span : (c + 1) * span] = jnp.where(mask, q, jnp.zeros_like(q))

    def groups(a):
        return a.reshape(a.shape[0] // 8, 8, a.shape[1])

    def score(d, slot, m8):
        q = qscr[d].astype(F32) * (KD**-0.5 * LOG2E)
        high = q.astype(BF16)
        rest = (q - high.astype(F32)).astype(BF16)
        k = kscr[...]
        s = jnp.dot(
            jnp.concatenate([k, k], axis=1),
            jnp.concatenate([high, rest], axis=0),
            preferred_element_type=F32,
        )
        sscr[slot] = s
        return jnp.maximum(m8, jnp.max(groups(s), axis=0))

    low = jnp.full((8, wide), -1e30, F32)

    def body(d, m8):
        m = jnp.broadcast_to(jnp.max(m8, axis=0, keepdims=True), m8.shape)
        p = jnp.exp2(groups(sscr[d % 2]) - m[None])
        mass = jnp.sum(p, axis=0)
        acc = jnp.dot(vscr[...], p.reshape(keys, wide).astype(BF16), preferred_element_type=F32)
        if not first:
            fix = jnp.exp2(carry_in[0][d] - m)
            mass = mass + carry_in[1][d] * fix
            acc = acc + (groups(carry_in[2][d]) * fix[None]).reshape(VD, wide)
        after = jnp.minimum(d + 1, nq - 1)
        m8 = score(after, (d + 1) % 2, low if first else carry_in[0][after])
        if last:
            lam, gain = extra
            read = acc / jnp.sum(mass, axis=0, keepdims=True)
            diff = read[:, :span] - lam[0] * read[:, span:]
            inv = lax.rsqrt(jnp.mean(diff * diff, axis=0, keepdims=True) + 1e-05)
            outs[0][d] = (diff * inv * gain[...]).T.astype(BF16)
        else:
            outs[0][d] = m
            outs[1][d] = mass
            outs[2][d] = acc
        return m8

    lax.fori_loop(0, nq, body, score(0, 0, low if first else carry_in[0][0]))


def attend(qs, kvs, carry, finish, span):
    nq = len(qs)
    counts = tuple(kv.shape[0] for kv in kvs)
    total = sum(counts)
    first, last = carry is None, finish is not None
    args = [*qs, *kvs, *(carry or ()), *(finish or ())]
    specs = [whole_spec() for _ in args]
    if last:
        specs[-2] = smem_spec()
        out_shape = [jax.ShapeDtypeStruct((nq, span, VD), BF16)]
    else:
        out_shape = [
            jax.ShapeDtypeStruct((nq, 8, 2 * span), F32),
            jax.ShapeDtypeStruct((nq, 8, 2 * span), F32),
            jax.ShapeDtypeStruct((nq, VD, 2 * span), F32),
        ]
    cells = nq * 2 * span * total * span
    return pl.pallas_call(
        functools.partial(
            attend_body, nq=nq, span=span, counts=counts, first=first, last=last
        ),
        in_specs=specs,
        out_specs=[whole_spec() for _ in out_shape],
        out_shape=out_shape,
        scratch_shapes=[
            pltpu.VMEM((total * span, VD), BF16),
            pltpu.VMEM((VD, total * span), BF16),
            pltpu.VMEM((nq, 2 * KD, 2 * span), BF16),
            pltpu.VMEM((2, total * span, 2 * span), F32),
        ],
        cost_estimate=pl.CostEstimate(
            flops=cells * 2 * (2 * KD + VD), transcendentals=cells, bytes_accessed=4 * VD * cells // span
        ),
        compiler_params=pltpu.CompilerParams(vmem_limit_bytes=14 * MIB),
        name="attend",
    )(*args)


def output_body(zi, *refs):
    out, scr = refs[-2:]
    weights = refs[-4:-2]
    pieces = refs[:-4]
    heads = len(pieces) // 2

    @pl.when(pl.program_id(0) == 0)
    def _():
        for index, piece in enumerate(pieces):
            side, d = divmod(index, heads)
            head = jnp.bitwise_xor(zi[0], d)
            scr[side, :, pl.ds(pl.multiple_of(head * VD, VD), VD)] = piece[...]

    total = jnp.dot(scr[0], weights[0][...], preferred_element_type=F32)
    total = total + jnp.dot(scr[1], weights[1][...], preferred_element_type=F32)
    out[...] = total.astype(BF16)


def output(zi, own, other, w_own, w_other):
    span = own[0].shape[0]
    rows, width = w_own.shape
    tile = 512
    fixed = lambda i, z: (0, 0)
    piece = pl.BlockSpec((span, VD), fixed)
    weight = pl.BlockSpec((rows, tile), lambda i, z: (0, i))
    return pl.pallas_call(
        output_body,
        grid_spec=pltpu.PrefetchScalarGridSpec(
            num_scalar_prefetch=1,
            grid=(width // tile,),
            in_specs=[piece] * (2 * len(own)) + [weight, weight],
            out_specs=pl.BlockSpec((span, tile), lambda i, z: (0, i)),
            scratch_shapes=[pltpu.VMEM((2, span, rows), BF16)],
        ),
        out_shape=jax.ShapeDtypeStruct((span, width), BF16),
        compiler_params=pltpu.CompilerParams(
            dimension_semantics=("arbitrary",), vmem_limit_bytes=10 * MIB
        ),
        name="output",
    )(zi, *own, *other, w_own, w_other)


def shards(tokens, in_gain, w_query, w_key, w_value, lam, sub_gain, w_out, *, size, tp):
    span = tokens.shape[0]
    heads = lam.shape[0]
    split = heads if heads & (heads - 1) == 0 and size % heads == 0 else 1
    rest = size // split
    where = lax.axis_index("sp")
    flip = [(0, 1), (1, 0)]
    special = size == 16 and heads == 4 and tp == 2
    zi = (where // 4) % 2 * 2 + where % 2 if special else where // rest

    def swap_far(a, d):
        return lax.ppermute(
            a, "sp", [(i, ((i // rest) ^ d) * rest + i % rest) for i in range(size)]
        )

    index = zi.astype(jnp.int32)[None] if split == heads else jnp.zeros((1,), jnp.int32)
    place = jnp.concatenate([index, (where * span).astype(jnp.int32)[None]])
    parts = project(place, tokens, in_gain, w_query, w_key, w_value, heads)
    gain = sub_gain[:, None]

    if split == heads:
        if special:
            lam_other = lax.ppermute(lam, "tp", flip)
            same = (where // 2) % 2 == lax.axis_index("tp")
            lam_mine = lax.dynamic_slice_in_dim(jnp.where(same, lam, lam_other), index[0], 1)

            def far(a, d, c):
                pairs = []
                for i in range(size):
                    y, swap = (i // 2) % 2, i ^ (8 * c) ^ (4 * (d // 2)) ^ (d % 2)
                    for t in range(2):
                        pairs.append((2 * i + t, 2 * ((swap & ~2) | (2 * t)) + y))
                return lax.ppermute(a, ("sp", "tp"), pairs)

            def cross(a):
                return lax.ppermute(a, "tp", flip)

            order = range(heads)
            mine = [far(parts[d], d, 0) for d in order]
            away = [far(parts[d, : 2 * span], d, 1) for d in order]
            here = jnp.stack([a[: 2 * span] for a in mine])
            side = cross(here)
            one, two = jnp.stack(away[:2]), jnp.stack(away[2:])
            cross_one, cross_two = cross(one), cross(two)
            carry = attend(mine, [here], None, None, span)
            carry = attend(mine, [side], carry, None, span)
            carry = attend(mine, [one, cross_one], carry, None, span)
            done = attend(mine, [two, cross_two], carry, (lam_mine, gain), span)[0]
            own = [far(done[d], d, 0) for d in order]
        else:
            lam_mine = lax.dynamic_slice_in_dim(lam, index[0], 1)
            finish = (lam_mine, gain)
            mine = [parts[0]] + [swap_far(parts[d], d) for d in range(1, heads)]
            kv = jnp.stack([a[: 2 * span] for a in mine])
            groups = [[g * rest + r for r in range(rest)] for g in range(split)]
            kw = {} if split == 1 else {"axis_index_groups": groups}
            every = lax.all_gather(kv, "sp", axis=0, tiled=True, **kw)
            carry = None
            for at in range(0, every.shape[0], 4):
                end = finish if at + 4 >= every.shape[0] else None
                carry = attend(mine, [every[at : at + 4]], carry, end, span)
            own = [carry[0][0]] + [swap_far(carry[0][d], d) for d in range(1, heads)]
    else:
        own = []
        for h in range(heads):
            every = lax.all_gather(parts[h][None, : 2 * span], "sp", axis=0, tiled=True)
            carry = None
            for at in range(0, size, 4):
                end = (lam[h : h + 1], gain) if at + 4 >= size else None
                carry = attend([parts[h]], [every[at : at + 4]], carry, end, span)
            own.append(carry[0][0])

    if tp == 2:
        w_other = lax.ppermute(w_out, "tp", flip)
        other = lax.ppermute(jnp.stack(own), "tp", flip)
        other = [other[d] for d in range(heads)]
        return output(index, own, other, w_out, w_other)
    attended = jnp.concatenate(own, axis=1)
    if tp > 1:
        attended = lax.all_gather(attended, "tp", axis=1, tiled=True)
        w_out = lax.all_gather(w_out, "tp", axis=0, tiled=True)
    return jnp.dot(attended, w_out, preferred_element_type=F32).astype(BF16)


def solution(mesh):
    in_specs = (
        P("sp", None),
        P(),
        P(None, "tp"),
        P(None, "tp"),
        P(None, "tp"),
        P("tp"),
        P(),
        P("tp", None),
    )

    def body(*args):
        return shards(*args, size=mesh.shape["sp"], tp=mesh.shape["tp"])

    return jax.shard_map(
        body, mesh=mesh, in_specs=in_specs, out_specs=P("sp", None), check_vma=False
    )
```
